32 devices in a mesh: dp: 4 (over y, x), kv: 4 (over z), tp: 2 (over core).
Axes of the slice: x: 2, y: 2, z: 4, core: 2. Of those that a mesh axis runs over, the one named last changes fastest.
Arguments:
- tokens: bfloat16 [16, 4096], P('dp', ('kv', 'tp')), may hold values from -24 to 24
- rec_state: float32 [16, 16, 128, 128], P(('dp', 'kv'), 'tp'), may hold values from -2 to 2
- norm_gain: float32 [4096], replicated, may hold values from 0.1 to 1.9
- w_query: bfloat16 [4096, 2048], P('kv', 'tp'), may hold values from -0.09375 to 0.09375
- w_forget: bfloat16 [4096, 2048], P('kv', 'tp'), may hold values from -0.09375 to 0.09375
- w_input: bfloat16 [4096, 2048], P('kv', 'tp'), may hold values from -0.09375 to 0.09375
- w_outgate: bfloat16 [4096, 2048], P('kv', 'tp'), may hold values from -0.09375 to 0.09375
- lower_bound: float32 [2048], P('tp'), may hold values from 0 to 0.9
- head_gain: float32 [2048], P('tp'), may hold values from 0.1 to 1.9
- w_heads_out: bfloat16 [2048, 4096], P(None, ('kv', 'tp')), may hold values from -0.125 to 0.125
- mixer_gain: float32 [4096], replicated, may hold values from 0.1 to 1.9
- w_gate: bfloat16 [4096, 11264], P(None, ('kv', 'tp')), may hold values from -0.09375 to 0.09375
- w_up: bfloat16 [4096, 11264], P(None, ('kv', 'tp')), may hold values from -0.09375 to 0.09375
- w_down: bfloat16 [11264, 4096], P(('kv', 'tp')), may hold values from -0.078125 to 0.078125
Outputs:
- result: bfloat16 [16, 4096], P('dp', ('kv', 'tp'))
- new_state: float32 [16, 16, 128, 128], P(('dp', 'kv'), 'tp')
The draws below stay inside these ranges and needn't reach their ends.
All inputs are finite; a program needn't handle non-finite values.
Results may differ from the reference program's by a relative error of at most 0.012.
Values may be sent and summed in bfloat16 or wider, within the bound.
A program may use at most 128 MiB of HBM per device.

```python
import math
import jax
import jax.numpy as jnp
from jax import lax

D = 4096
HEAD_DIM = 128
HEADS = 16
FF = 11264
HG = 2048
BATCH = 16


def draw_tokens(key, part):
    key_rows = jax.random.fold_in(key, 11)
    key_vals = jax.random.fold_in(key, 12)
    col_scale = jnp.exp(jnp.linspace(math.log(0.5), math.log(2.0), D))[None, :]
    row_scale = jnp.exp(jax.random.uniform(key_rows, (BATCH, 1), jnp.float32, math.log(0.3), math.log(3.0)))
    values = jnp.clip(jax.random.normal(key_vals, (BATCH, D), jnp.float32), -4.0, 4.0)
    return (values * row_scale * col_scale).astype(jnp.bfloat16)


def strengthened(array, own_key, source, target, parts, factor):
    owner, partner = [(jnp.arange(array.shape[dim]) // (array.shape[dim] // parts)).reshape([-1 if axis == dim else 1 for axis in range(array.ndim)]) for dim in (source, target)]
    chosen = jax.random.permutation(own_key, parts)[partner]
    strong = (owner == chosen) | (owner == (partner + parts // 2) % parts)
    return jnp.where(strong, factor * array, array)


def block_levels(rng, shape, shards, least, top_value):
    loudness = 1.0
    for axis_at, parts in shards:
        steps = jax.random.uniform(jax.random.fold_in(jax.random.fold_in(rng, 6), axis_at), (parts,), jnp.float32, least / len(shards), top_value / len(shards))
        loudness = loudness * jnp.repeat(jnp.exp(steps), shape[axis_at] // parts).reshape((-1,) + (1,) * (len(shape) - 1 - axis_at))
    return loudness


def gaussian(key, extent, deviation, limit, shards=(), kind=jnp.bfloat16):
    drawn = deviation * jax.random.normal(key, extent, jnp.float32)
    if shards:
        drawn = drawn * block_levels(key, extent, shards, -0.22, 0.18)
    return jnp.clip(drawn, -limit, limit).astype(kind)


def noise_with(stream_key, shape, scale, bound, split, heavy, held_as=jnp.bfloat16):
    array = scale * jax.random.normal(stream_key, shape, jnp.float32)
    if split:
        array = array * block_levels(stream_key, shape, split, -0.22, 0.18)
    return jnp.clip(strengthened(array, jax.random.fold_in(stream_key, 3), *heavy), -bound, bound).astype(held_as)


def setup_inputs(seed: int = 0) -> dict:
    streams_of = jax.random.split(jax.random.key(seed), 15)
    return {
        "tokens": draw_tokens(jax.random.fold_in(streams_of[14], 71), 0),
        "rec_state": gaussian(streams_of[1], (BATCH, HEADS, HEAD_DIM, HEAD_DIM), 0.3, 2.0, ((0, 16), (1, 2)), jnp.float32),
        "norm_gain": jnp.clip(1.0 + 0.18 * jax.random.normal(streams_of[2], (D,), jnp.float32), 0.1, 1.9),
        "w_query": gaussian(streams_of[3], (D, HG), D ** -0.5, 0.09375, ((0, 4), (1, 2))),
        "w_forget": gaussian(streams_of[4], (D, HG), D ** -0.5, 0.09375, ((0, 4), (1, 2))),
        "w_input": gaussian(streams_of[5], (D, HG), D ** -0.5, 0.09375, ((0, 4), (1, 2))),
        "w_outgate": gaussian(streams_of[6], (D, HG), D ** -0.5, 0.09375, ((0, 4), (1, 2))),
        "lower_bound": jnp.clip(0.9 * jax.random.uniform(streams_of[7], (HG,), jnp.float32) ** block_levels(streams_of[7], (HG,), ((0, 2),), -0.2, 0.2), 0.0, 0.9),
        "head_gain": jnp.clip(1.0 + 0.18 * jax.random.normal(streams_of[8], (HG,), jnp.float32), 0.1, 1.9),
        "w_heads_out": gaussian(streams_of[9], (HG, D), HG ** -0.5, 0.125, ((1, 8),)),
        "mixer_gain": jnp.clip(1.0 + 0.18 * jax.random.normal(streams_of[10], (D,), jnp.float32), 0.1, 1.9),
        "w_gate": gaussian(streams_of[11], (D, FF), D ** -0.5, 0.09375, ((1, 8),)),
        "w_up": gaussian(streams_of[12], (D, FF), D ** -0.5, 0.09375, ((1, 8),)),
        "w_down": noise_with(streams_of[13], (FF, D), FF ** -0.5, 0.078125, ((0, 8),), (0, 1, 8, 2.0)),
    }


epsilon = 1e-06

def reference(tokens, rec_state, norm_gain, w_query, w_forget, w_input, w_outgate, lower_bound, head_gain, w_heads_out, mixer_gain, w_gate, w_up, w_down):
    tok_float = tokens.astype(jnp.float32)
    row_scale = lax.rsqrt(lax.optimization_barrier(jnp.mean(tok_float * tok_float, axis=1, keepdims=True)) + epsilon)
    scaled = (tok_float * norm_gain).astype(jnp.bfloat16)
    query_pre = row_scale * jnp.dot(scaled, w_query, preferred_element_type=jnp.float32)
    forget_pre = row_scale * jnp.dot(scaled, w_forget, preferred_element_type=jnp.float32)
    value_in = row_scale * jnp.dot(scaled, w_input, preferred_element_type=jnp.float32)
    gate_pre = row_scale * jnp.dot(scaled, w_outgate, preferred_element_type=jnp.float32)
    forget = lower_bound + (1.0 - lower_bound) * jax.nn.sigmoid(forget_pre)
    key_in = 1.0 - forget
    query_act = jax.nn.silu(query_pre)
    batch_rows = tokens.shape[0]
    shaped = (batch_rows, HEADS, HEAD_DIM)
    forget = forget.reshape(shaped)
    key_in = key_in.reshape(shaped)
    value_in = value_in.reshape(shaped)
    query_act = query_act.reshape(shaped)
    new_state = forget[:, :, :, None] * rec_state + key_in[:, :, :, None] * value_in[:, :, None, :]
    head_out = lax.optimization_barrier(jnp.sum(query_act[:, :, :, None] * new_state, axis=2))
    head_out = head_out * lax.rsqrt(lax.optimization_barrier(jnp.mean(head_out * head_out, axis=2, keepdims=True)) + epsilon)
    head_out = head_out * head_gain.reshape(HEADS, HEAD_DIM)
    gated = (head_out.reshape(batch_rows, HG) * jax.nn.silu(gate_pre)).astype(jnp.bfloat16)
    mixed = (tok_float + jnp.dot(gated, w_heads_out, preferred_element_type=jnp.float32)).astype(jnp.bfloat16)
    mixed_float = mixed.astype(jnp.float32)
    mixer_scale = lax.rsqrt(lax.optimization_barrier(jnp.mean(mixed_float * mixed_float, axis=1, keepdims=True)) + epsilon)
    normed = (mixed_float * mixer_scale * mixer_gain).astype(jnp.bfloat16)
    gate_val = jnp.dot(normed, w_gate, preferred_element_type=jnp.float32)
    up_val = jnp.dot(normed, w_up, preferred_element_type=jnp.float32)
    hidden = (jax.nn.silu(gate_val) * up_val).astype(jnp.bfloat16)
    result = (mixed_float + jnp.dot(hidden, w_down, preferred_element_type=jnp.float32)).astype(jnp.bfloat16)
    return (result, new_state)
```

```python
import functools

import jax
import jax.numpy as jnp
from jax import lax
from jax.experimental import pallas as pl
from jax.experimental.pallas import tpu as pltpu
from jax.sharding import PartitionSpec as P

HEAD_DIM = 128


epsilon = 1e-06


def channel_mixer(whole_rows, mixer_gain, w_gate, w_up, w_down):
    rows_float = whole_rows.astype(jnp.float32)
    mixer_scale = lax.rsqrt(jnp.mean(rows_float * rows_float, axis=1, keepdims=True) + epsilon)
    normed = (rows_float * mixer_scale * mixer_gain).astype(jnp.bfloat16)
    gate_val = jnp.dot(normed, w_gate, preferred_element_type=jnp.float32)
    up_val = jnp.dot(normed, w_up, preferred_element_type=jnp.float32)
    hidden = (jax.nn.silu(gate_val) * up_val).astype(jnp.bfloat16)
    return jnp.dot(hidden, w_down, preferred_element_type=jnp.float32)


def local_plain(
    tokens,
    rec_state,
    norm_gain,
    w_query,
    w_forget,
    w_input,
    w_outgate,
    lower_bound,
    head_gain,
    w_heads_out,
    mixer_gain,
    w_gate,
    w_up,
    w_down,
):
    kv_count = lax.axis_size("kv")
    tp_count = lax.axis_size("tp")
    kv_index = lax.axis_index("kv")
    row_count = tokens.shape[0]
    seq_count = rec_state.shape[0]
    model_width = norm_gain.shape[0]
    col_block = model_width // kv_count
    tok_float = tokens.astype(jnp.float32)
    whole_rows = lax.all_gather(tokens, ("kv", "tp"), axis=1, tiled=True).astype(jnp.float32)
    squares = jnp.sum(whole_rows * whole_rows, axis=1)
    own_cols = lax.dynamic_slice_in_dim(whole_rows, kv_index * col_block, col_block, 1)
    gain_block = lax.dynamic_slice_in_dim(norm_gain, kv_index * col_block, col_block, 0)
    scaled = (own_cols * gain_block).astype(jnp.bfloat16)
    projected = lax.psum_scatter(
        jnp.stack(
            [
                jnp.dot(scaled, weight, preferred_element_type=jnp.float32)
                for weight in (w_query, w_forget, w_input, w_outgate)
            ],
            axis=1,
        ),
        "kv",
        scatter_dimension=0,
        tiled=True,
    )
    my_squares = lax.dynamic_slice_in_dim(squares, kv_index * seq_count, seq_count, 0)
    row_scale = lax.rsqrt(my_squares / model_width + epsilon)[:, None]
    query_pre = row_scale * projected[:, 0]
    forget_pre = row_scale * projected[:, 1]
    value_in = row_scale * projected[:, 2]
    gate_pre = row_scale * projected[:, 3]
    forget = lower_bound + (1.0 - lower_bound) * jax.nn.sigmoid(forget_pre)
    key_in = 1.0 - forget
    query_act = jax.nn.silu(query_pre)
    head_count = rec_state.shape[1]
    shaped = (seq_count, head_count, HEAD_DIM)
    forget = forget.reshape(shaped)
    key_in = key_in.reshape(shaped)
    value_in = value_in.reshape(shaped)
    query_act = query_act.reshape(shaped)
    new_state = forget[:, :, :, None] * rec_state + key_in[:, :, :, None] * value_in[:, :, None, :]
    head_out = jnp.sum(query_act[:, :, :, None] * new_state, axis=2)
    head_out = head_out * lax.rsqrt(jnp.mean(head_out * head_out, axis=2, keepdims=True) + epsilon)
    head_out = head_out * head_gain.reshape(head_count, HEAD_DIM)
    local_width = head_count * HEAD_DIM
    gated = (head_out.reshape(seq_count, local_width) * jax.nn.silu(gate_pre)).astype(jnp.bfloat16)
    every_head = lax.all_gather(gated[None], ("kv", "tp"), axis=0, tiled=True)
    every_head = every_head.reshape(kv_count, tp_count, seq_count, local_width)
    every_head = every_head.transpose(0, 2, 1, 3).reshape(
        kv_count * seq_count, tp_count * local_width
    )
    mixed_add = jnp.dot(every_head, w_heads_out, preferred_element_type=jnp.float32)
    mixed = (tok_float + mixed_add).astype(jnp.bfloat16)
    gathered = lax.all_gather(mixed, ("kv", "tp"), axis=1, tiled=True)
    terms = channel_mixer(gathered, mixer_gain, w_gate, w_up, w_down)
    out_block = model_width // (kv_count * tp_count)
    blocked = terms.reshape(row_count, kv_count, tp_count, out_block)
    chip_sum = lax.psum_scatter(blocked.astype(jnp.bfloat16), "tp", scatter_dimension=2, tiled=True)
    down_sum = (
        lax.psum_scatter(chip_sum, "kv", scatter_dimension=1, tiled=True)
        .astype(jnp.float32)
        .reshape(row_count, out_block)
    )
    result = (mixed.astype(jnp.float32) + down_sum).astype(jnp.bfloat16)
    return (result, new_state)


LANES = 128
MESH = pl.DeviceIdType.MESH


def silu(v):
    return v / (1.0 + jnp.exp(-v))


def layer_kernel(
    kv_count,
    tp_count,
    tokens,
    rec_state,
    norm_gain,
    w_query,
    w_forget,
    w_input,
    w_outgate,
    lower_bound,
    head_gain,
    w_heads_out,
    mixer_gain,
    w_gate,
    w_up,
    w_down,
    result,
    new_state,
    tok_all,
    state_in,
    state_out,
    ngain_buf,
    lower_buf,
    hgain_buf,
    mgain_buf,
    proj_w,
    heads_w,
    gate_w,
    up_w,
    down_w,
    proj_send,
    proj_recv,
    head_rows,
    gated_all,
    gated_float,
    mixed_all,
    gate_acc,
    up_acc,
    hidden_buf,
    down_send,
    down_recv,
    small_sem,
    proj_sem,
    heads_sem,
    gate_sem,
    up_sem,
    down_sem,
    tok_ssem,
    tok_rsem,
    proj_ssem,
    proj_rsem,
    gated_ssem,
    gated_rsem,
    mixed_ssem,
    mixed_rsem,
    red_ssem,
    red_rsem,
):
    kv = lax.axis_index("kv")
    tp = lax.axis_index("tp")
    group = kv_count * tp_count
    me = kv * tp_count + tp
    rows, cols = tokens.shape
    head_count = rec_state.shape[1]
    width = cols * group
    proj_rows = cols * tp_count

    def coords(index):
        return {"kv": lax.div(index, tp_count), "tp": lax.rem(index, tp_count)}

    def ahead(step):
        return lax.rem(me + step, group)

    def behind(step):
        return lax.rem(me + group - step, group)

    def rows_of(step):
        return pl.ds(pl.multiple_of(behind(step) * cols, LANES), cols)

    def cols_of(step):
        return pl.ds(pl.multiple_of(ahead(step) * cols, LANES), cols)

    tok_copy = pltpu.make_async_copy(tokens, tok_all.at[tp], small_sem.at[0])
    small_copies = [
        pltpu.make_async_copy(norm_gain, ngain_buf, small_sem.at[1]),
        pltpu.make_async_copy(lower_bound, lower_buf, small_sem.at[2]),
        pltpu.make_async_copy(head_gain, hgain_buf, small_sem.at[3]),
        pltpu.make_async_copy(mixer_gain, mgain_buf, small_sem.at[4]),
    ]
    state_copy = pltpu.make_async_copy(rec_state.at[0], state_in, small_sem.at[5])
    proj_copies = [
        pltpu.make_async_copy(weight, proj_w.at[i], proj_sem.at[i])
        for i, weight in enumerate((w_query, w_forget, w_input, w_outgate))
    ]
    heads_copy = pltpu.make_async_copy(w_heads_out, heads_w, heads_sem)

    def gate_copy(step):
        return pltpu.make_async_copy(w_gate.at[rows_of(step), :], gate_w.at[step], gate_sem.at[step])

    def up_copy(step):
        return pltpu.make_async_copy(w_up.at[rows_of(step), :], up_w.at[step], up_sem.at[step])

    def down_copy(step):
        return pltpu.make_async_copy(w_down.at[:, cols_of(step)], down_w.at[step], down_sem.at[step])

    tok_copy.start()
    for copy in small_copies:
        copy.start()
    for copy in proj_copies:
        copy.start()
    state_copy.start()
    heads_copy.start()

    barrier = pltpu.get_barrier_semaphore()
    for step in range(1, group):
        pl.semaphore_signal(barrier, inc=1, device_id=coords(ahead(step)), device_id_type=MESH)
    for step in range(group):
        gate_copy(step).start()
        up_copy(step).start()
    for step in range(group):
        down_copy(step).start()
    pl.semaphore_wait(barrier, group - 1)

    tok_copy.wait()
    tok_sends = []
    for step in range(1, tp_count):
        send = pltpu.make_async_remote_copy(
            src_ref=tok_all.at[tp],
            dst_ref=tok_all.at[tp],
            send_sem=tok_ssem.at[step],
            recv_sem=tok_rsem.at[step],
            device_id={"tp": lax.rem(tp + step, tp_count)},
            device_id_type=MESH,
        )
        send.start()
        tok_sends.append(send)
    for copy in small_copies:
        copy.wait()
    for step in range(1, tp_count):
        source = lax.rem(tp + tp_count - step, tp_count)
        pltpu.make_async_remote_copy(
            src_ref=tok_all.at[source],
            dst_ref=tok_all.at[source],
            send_sem=tok_ssem.at[step],
            recv_sem=tok_rsem.at[step],
            device_id={"tp": source},
            device_id_type=MESH,
        ).wait_recv()

    tok_float = jnp.concatenate([tok_all[i].astype(jnp.float32) for i in range(tp_count)], axis=1)
    squares = jnp.sum(tok_float * tok_float, axis=1, keepdims=True)
    per_block = proj_rows // LANES
    gain_row = jnp.concatenate(
        [ngain_buf[pl.ds(kv * per_block + i, 1), :] for i in range(per_block)], axis=1
    )
    scaled = (tok_float * gain_row).astype(jnp.bfloat16)
    square_rows = jnp.broadcast_to(squares, (rows, LANES))
    for h in range(head_count):
        proj_send[:, 4, h, :] = square_rows

    @pl.loop(0, 4)
    def _(which):
        pltpu.make_async_copy(w_query, proj_w.at[which], proj_sem.at[which]).wait()
        part = jnp.dot(scaled, proj_w[which], preferred_element_type=jnp.float32)
        for h in range(head_count):
            proj_send[:, which, h, :] = part[:, h * LANES : (h + 1) * LANES]

    proj_sends = []
    for step in range(1, kv_count):
        target = lax.rem(kv + step, kv_count)
        send = pltpu.make_async_remote_copy(
            src_ref=proj_send.at[target],
            dst_ref=proj_recv.at[step],
            send_sem=proj_ssem.at[step],
            recv_sem=proj_rsem.at[step],
            device_id={"kv": target},
            device_id_type=MESH,
        )
        send.start()
        proj_sends.append(send)
    total = proj_send[kv]
    state_copy.wait()
    for step in range(1, kv_count):
        proj_sends[step - 1].wait_recv()
        total = total + proj_recv[step]
    row_scale = lax.rsqrt(total[4] / width + epsilon)
    query_act = silu(row_scale * total[0])
    lower = lower_buf[...]
    forget = lower + (1.0 - lower) / (1.0 + jnp.exp(-(row_scale * total[1])))
    key_in = 1.0 - forget
    value_in = row_scale * total[2]
    gate_act = silu(row_scale * total[3])
    forget_t = forget.T
    key_t = key_in.T
    query_t = query_act.T
    for h in range(head_count):
        fresh = forget_t[:, h : h + 1] * state_in[h] + key_t[:, h : h + 1] * value_in[h : h + 1, :]
        state_out[h] = fresh
        head_rows[h : h + 1, :] = jnp.sum(query_t[:, h : h + 1] * fresh, axis=0, keepdims=True)
    head_out = head_rows[...]
    head_out = head_out * lax.rsqrt(jnp.mean(head_out * head_out, axis=1, keepdims=True) + epsilon)
    gated_all[0] = (head_out * hgain_buf[...] * gate_act).astype(jnp.bfloat16)

    gated_sends = []
    for step in range(1, group):
        send = pltpu.make_async_remote_copy(
            src_ref=gated_all.at[0],
            dst_ref=gated_all.at[step],
            send_sem=gated_ssem.at[step],
            recv_sem=gated_rsem.at[step],
            device_id=coords(ahead(step)),
            device_id_type=MESH,
        )
        send.start()
        gated_sends.append(send)
    state_store = pltpu.make_async_copy(state_out, new_state.at[0], small_sem.at[6])
    state_store.start()
    gated_float[kv, tp] = gated_all[0].astype(jnp.float32)
    heads_copy.wait()
    for step in range(1, group):
        gated_sends[step - 1].wait_recv()
        source = behind(step)
        gated_float[lax.div(source, tp_count), lax.rem(source, tp_count)] = gated_all[step].astype(jnp.float32)
    every_head = jnp.concatenate(
        [gated_float[:, t, h, :] for t in range(tp_count) for h in range(head_count)], axis=1
    ).astype(jnp.bfloat16)
    mixed_add = jnp.dot(every_head, heads_w[...], preferred_element_type=jnp.float32)
    mixed = (tok_all[tp].astype(jnp.float32) + mixed_add).astype(jnp.bfloat16)
    mixed_all[0] = mixed

    mixed_sends = []
    for step in range(1, group):
        send = pltpu.make_async_remote_copy(
            src_ref=mixed_all.at[0],
            dst_ref=mixed_all.at[step],
            send_sem=mixed_ssem.at[step],
            recv_sem=mixed_rsem.at[step],
            device_id=coords(ahead(step)),
            device_id_type=MESH,
        )
        send.start()
        mixed_sends.append(send)

    gate_acc[...] = jnp.zeros_like(gate_acc)
    up_acc[...] = jnp.zeros_like(up_acc)
    per_cols = cols // LANES

    def mixer_step(step, squares_sum):
        mixed_float = mixed_all[step].astype(jnp.float32)
        gain = jnp.concatenate(
            [mgain_buf[pl.ds(behind(step) * per_cols + i, 1), :] for i in range(per_cols)], axis=1
        )
        weighted = (mixed_float * gain).astype(jnp.bfloat16)
        gate_copy(step).wait()
        gate_acc[...] += jnp.dot(weighted, gate_w[step], preferred_element_type=jnp.float32)
        up_copy(step).wait()
        up_acc[...] += jnp.dot(weighted, up_w[step], preferred_element_type=jnp.float32)
        return squares_sum + jnp.sum(mixed_float * mixed_float, axis=1, keepdims=True)

    def mixer_arrived(step, squares_sum):
        pltpu.make_async_remote_copy(
            src_ref=mixed_all.at[0],
            dst_ref=mixed_all.at[step],
            send_sem=mixed_ssem.at[step],
            recv_sem=mixed_rsem.at[step],
            device_id=coords(ahead(step)),
            device_id_type=MESH,
        ).wait_recv()
        return mixer_step(step, squares_sum)

    squares_sum = mixer_step(0, jnp.zeros((rows, 1), jnp.float32))
    squares_sum = lax.fori_loop(1, group, mixer_arrived, squares_sum)
    mixer_scale = lax.rsqrt(squares_sum / width + epsilon)
    hidden_buf[...] = (silu(mixer_scale * gate_acc[...]) * (mixer_scale * up_acc[...])).astype(jnp.bfloat16)

    def down_part(step):
        down_copy(step).wait()
        return jnp.dot(hidden_buf[...], down_w[step], preferred_element_type=jnp.float32)

    def red_send(step):
        return pltpu.make_async_remote_copy(
            src_ref=down_send.at[step],
            dst_ref=down_recv.at[step],
            send_sem=red_ssem.at[step],
            recv_sem=red_rsem.at[step],
            device_id=coords(ahead(step)),
            device_id_type=MESH,
        )

    @pl.loop(1, group)
    def _(step):
        down_send[step] = down_part(step).astype(jnp.bfloat16)
        red_send(step).start()

    final = mixed.astype(jnp.float32) + down_part(0)
    for step in range(1, group):
        red_send(step).wait_recv()
        final = final + down_recv[step].astype(jnp.float32)
    result[...] = final.astype(jnp.bfloat16)
    state_store.wait()
    for send in tok_sends + proj_sends + gated_sends + mixed_sends:
        send.wait_send()
    for step in range(1, group):
        red_send(step).wait_send()


def local(
    kv_count,
    tp_count,
    tokens,
    rec_state,
    norm_gain,
    w_query,
    w_forget,
    w_input,
    w_outgate,
    lower_bound,
    head_gain,
    w_heads_out,
    mixer_gain,
    w_gate,
    w_up,
    w_down,
):
    group = kv_count * tp_count
    rows, cols = tokens.shape
    head_count = rec_state.shape[1]
    hidden = w_gate.shape[1]
    model_width = norm_gain.shape[0]
    head_width = head_count * HEAD_DIM
    fits = (
        rec_state.shape[0] == 1
        and HEAD_DIM == LANES
        and head_count % 8 == 0
        and cols % LANES == 0
        and hidden % LANES == 0
        and w_down.shape[0] == hidden
    )
    if not fits:
        return local_plain(
            tokens, rec_state, norm_gain, w_query, w_forget, w_input, w_outgate, lower_bound,
            head_gain, w_heads_out, mixer_gain, w_gate, w_up, w_down,
        )
    f32, bf16 = jnp.float32, jnp.bfloat16
    dma = pltpu.SemaphoreType.DMA
    vmem = pltpu.VMEM
    scratch = [
        vmem((tp_count, rows, cols), bf16),
        vmem(rec_state.shape[1:], f32),
        vmem(rec_state.shape[1:], f32),
        vmem((model_width // LANES, LANES), f32),
        vmem((head_count, LANES), f32),
        vmem((head_count, LANES), f32),
        vmem((model_width // LANES, LANES), f32),
        vmem((4,) + w_query.shape, bf16),
        vmem(w_heads_out.shape, bf16),
        vmem((group, cols, hidden), bf16),
        vmem((group, cols, hidden), bf16),
        vmem((group, hidden, cols), bf16),
        vmem((kv_count, 5, head_count, LANES), f32),
        vmem((kv_count, 5, head_count, LANES), f32),
        vmem((head_count, LANES), f32),
        vmem((group, head_count, LANES), bf16),
        vmem((kv_count, tp_count, head_count, LANES), f32),
        vmem((group, rows, cols), bf16),
        vmem((rows, hidden), f32),
        vmem((rows, hidden), f32),
        vmem((rows, hidden), bf16),
        vmem((group, rows, cols), bf16),
        vmem((group, rows, cols), bf16),
        dma((7,)),
        dma((4,)),
        dma,
        dma((group,)),
        dma((group,)),
        dma((group,)),
        dma((tp_count,)),
        dma((tp_count,)),
        dma((kv_count,)),
        dma((kv_count,)),
        dma((group,)),
        dma((group,)),
        dma((group,)),
        dma((group,)),
        dma((group,)),
        dma((group,)),
    ]
    return pl.pallas_call(
        functools.partial(layer_kernel, kv_count, tp_count),
        out_shape=(
            jax.ShapeDtypeStruct(tokens.shape, bf16),
            jax.ShapeDtypeStruct(rec_state.shape, f32),
        ),
        in_specs=[pl.BlockSpec(memory_space=pl.ANY)] * 14,
        out_specs=(
            pl.BlockSpec(memory_space=pltpu.VMEM),
            pl.BlockSpec(memory_space=pl.ANY),
        ),
        scratch_shapes=scratch,
        compiler_params=pltpu.CompilerParams(
            collective_id=0, has_side_effects=True, vmem_limit_bytes=60 * 1024 * 1024
        ),
    )(
        tokens,
        rec_state,
        norm_gain.reshape(-1, LANES),
        w_query,
        w_forget,
        w_input,
        w_outgate,
        lower_bound.reshape(-1, LANES),
        head_gain.reshape(-1, LANES),
        w_heads_out,
        mixer_gain.reshape(-1, LANES),
        w_gate,
        w_up,
        w_down,
    )


def solution(mesh):
    placed = (
        P("dp", ("kv", "tp")),
        P(("dp", "kv"), "tp", None, None),
        P(),
        P("kv", "tp"),
        P("kv", "tp"),
        P("kv", "tp"),
        P("kv", "tp"),
        P("tp"),
        P("tp"),
        P(None, ("kv", "tp")),
        P(),
        P(None, ("kv", "tp")),
        P(None, ("kv", "tp")),
        P(("kv", "tp"), None),
    )
    return jax.shard_map(
        functools.partial(local, mesh.shape["kv"], mesh.shape["tp"]),
        mesh=mesh,
        in_specs=placed,
        out_specs=(P("dp", ("kv", "tp")), P(("dp", "kv"), "tp", None, None)),
        check_vma=False,
    )
```

```python
import functools

import jax
import jax.numpy as jnp
from jax import lax
from jax.experimental import pallas as pl
from jax.experimental.pallas import tpu as pltpu
from jax.sharding import PartitionSpec as P

HEAD_DIM = 128


epsilon = 1e-06


def channel_mixer(whole_rows, mixer_gain, w_gate, w_up, w_down):
    rows_float = whole_rows.astype(jnp.float32)
    mixer_scale = lax.rsqrt(jnp.mean(rows_float * rows_float, axis=1, keepdims=True) + epsilon)
    normed = (rows_float * mixer_scale * mixer_gain).astype(jnp.bfloat16)
    gate_val = jnp.dot(normed, w_gate, preferred_element_type=jnp.float32)
    up_val = jnp.dot(normed, w_up, preferred_element_type=jnp.float32)
    hidden = (jax.nn.silu(gate_val) * up_val).astype(jnp.bfloat16)
    return jnp.dot(hidden, w_down, preferred_element_type=jnp.float32)


def local_plain(
    tokens,
    rec_state,
    norm_gain,
    w_query,
    w_forget,
    w_input,
    w_outgate,
    lower_bound,
    head_gain,
    w_heads_out,
    mixer_gain,
    w_gate,
    w_up,
    w_down,
):
    kv_count = lax.axis_size("kv")
    tp_count = lax.axis_size("tp")
    kv_index = lax.axis_index("kv")
    row_count = tokens.shape[0]
    seq_count = rec_state.shape[0]
    model_width = norm_gain.shape[0]
    col_block = model_width // kv_count
    tok_float = tokens.astype(jnp.float32)
    whole_rows = lax.all_gather(tokens, ("kv", "tp"), axis=1, tiled=True).astype(jnp.float32)
    squares = jnp.sum(whole_rows * whole_rows, axis=1)
    own_cols = lax.dynamic_slice_in_dim(whole_rows, kv_index * col_block, col_block, 1)
    gain_block = lax.dynamic_slice_in_dim(norm_gain, kv_index * col_block, col_block, 0)
    scaled = (own_cols * gain_block).astype(jnp.bfloat16)
    projected = lax.psum_scatter(
        jnp.stack(
            [
                jnp.dot(scaled, weight, preferred_element_type=jnp.float32)
                for weight in (w_query, w_forget, w_input, w_outgate)
            ],
            axis=1,
        ),
        "kv",
        scatter_dimension=0,
        tiled=True,
    )
    my_squares = lax.dynamic_slice_in_dim(squares, kv_index * seq_count, seq_count, 0)
    row_scale = lax.rsqrt(my_squares / model_width + epsilon)[:, None]
    query_pre = row_scale * projected[:, 0]
    forget_pre = row_scale * projected[:, 1]
    value_in = row_scale * projected[:, 2]
    gate_pre = row_scale * projected[:, 3]
    forget = lower_bound + (1.0 - lower_bound) * jax.nn.sigmoid(forget_pre)
    key_in = 1.0 - forget
    query_act = jax.nn.silu(query_pre)
    head_count = rec_state.shape[1]
    shaped = (seq_count, head_count, HEAD_DIM)
    forget = forget.reshape(shaped)
    key_in = key_in.reshape(shaped)
    value_in = value_in.reshape(shaped)
    query_act = query_act.reshape(shaped)
    new_state = forget[:, :, :, None] * rec_state + key_in[:, :, :, None] * value_in[:, :, None, :]
    head_out = jnp.sum(query_act[:, :, :, None] * new_state, axis=2)
    head_out = head_out * lax.rsqrt(jnp.mean(head_out * head_out, axis=2, keepdims=True) + epsilon)
    head_out = head_out * head_gain.reshape(head_count, HEAD_DIM)
    local_width = head_count * HEAD_DIM
    gated = (head_out.reshape(seq_count, local_width) * jax.nn.silu(gate_pre)).astype(jnp.bfloat16)
    every_head = lax.all_gather(gated[None], ("kv", "tp"), axis=0, tiled=True)
    every_head = every_head.reshape(kv_count, tp_count, seq_count, local_width)
    every_head = every_head.transpose(0, 2, 1, 3).reshape(
        kv_count * seq_count, tp_count * local_width
    )
    mixed_add = jnp.dot(every_head, w_heads_out, preferred_element_type=jnp.float32)
    mixed = (tok_float + mixed_add).astype(jnp.bfloat16)
    gathered = lax.all_gather(mixed, ("kv", "tp"), axis=1, tiled=True)
    terms = channel_mixer(gathered, mixer_gain, w_gate, w_up, w_down)
    out_block = model_width // (kv_count * tp_count)
    blocked = terms.reshape(row_count, kv_count, tp_count, out_block)
    chip_sum = lax.psum_scatter(blocked.astype(jnp.bfloat16), "tp", scatter_dimension=2, tiled=True)
    down_sum = (
        lax.psum_scatter(chip_sum, "kv", scatter_dimension=1, tiled=True)
        .astype(jnp.float32)
        .reshape(row_count, out_block)
    )
    result = (mixed.astype(jnp.float32) + down_sum).astype(jnp.bfloat16)
    return (result, new_state)


LANES = 128
MESH = pl.DeviceIdType.MESH


def silu(v):
    return v / (1.0 + jnp.exp(-v))


def layer_kernel(
    kv_count,
    tp_count,
    tokens,
    rec_state,
    norm_gain,
    w_query,
    w_forget,
    w_input,
    w_outgate,
    lower_bound,
    head_gain,
    w_heads_out,
    mixer_gain,
    w_gate,
    w_up,
    w_down,
    result,
    new_state,
    tok_all,
    state_in,
    ngain_buf,
    lower_buf,
    hgain_buf,
    mgain_buf,
    proj_w,
    heads_w,
    gate_w,
    up_w,
    down_w,
    proj_acc,
    proj_float,
    proj_send,
    proj_recv,
    square_send,
    square_recv,
    head_rows,
    gated_all,
    gated_float,
    mixed_all,
    gate_acc,
    up_acc,
    hidden_buf,
    down_send,
    down_recv,
    small_sem,
    proj_sem,
    heads_sem,
    gate_sem,
    up_sem,
    down_sem,
    tok_ssem,
    tok_rsem,
    square_ssem,
    square_rsem,
    proj_ssem,
    proj_rsem,
    gated_ssem,
    gated_rsem,
    mixed_ssem,
    mixed_rsem,
    red_ssem,
    red_rsem,
):
    kv = lax.axis_index("kv")
    tp = lax.axis_index("tp")
    group = kv_count * tp_count
    me = kv * tp_count + tp
    rows, cols = tokens.shape
    head_count = rec_state.shape[1]
    width = cols * group
    proj_rows = cols * tp_count

    def coords(index):
        return {"kv": lax.div(index, tp_count), "tp": lax.rem(index, tp_count)}

    def peer(step):
        other, bit = 0, 1
        while bit < group:
            other = other + lax.rem((me // bit) + (step // bit), 2) * bit
            bit = 2 * bit
        return other

    def rows_of(step):
        return pl.ds(pl.multiple_of(peer(step) * cols, LANES), cols)

    def cols_of(step):
        return pl.ds(pl.multiple_of(peer(step) * cols, LANES), cols)

    tok_copy = pltpu.make_async_copy(tokens, tok_all.at[tp], small_sem.at[0])
    small_copies = [
        pltpu.make_async_copy(norm_gain, ngain_buf, small_sem.at[1]),
        pltpu.make_async_copy(lower_bound, lower_buf, small_sem.at[2]),
        pltpu.make_async_copy(head_gain, hgain_buf, small_sem.at[3]),
        pltpu.make_async_copy(mixer_gain, mgain_buf, small_sem.at[4]),
    ]
    state_copy = pltpu.make_async_copy(rec_state.at[0], state_in, small_sem.at[5])

    def proj_copy(weight, step, which):
        source = lax.rem(tp + tp_count - step, tp_count)
        from_rows = pl.ds(pl.multiple_of(source * cols, LANES), cols)
        return pltpu.make_async_copy(
            weight.at[from_rows, :], proj_w.at[step, which], proj_sem.at[step, which]
        )

    heads_copy = pltpu.make_async_copy(w_heads_out, heads_w, heads_sem)

    def gate_copy(step):
        return pltpu.make_async_copy(w_gate.at[rows_of(step), :], gate_w.at[step], gate_sem.at[step])

    def up_copy(step):
        return pltpu.make_async_copy(w_up.at[rows_of(step), :], up_w.at[step], up_sem.at[step])

    def down_copy(step):
        return pltpu.make_async_copy(w_down.at[:, cols_of(step)], down_w.at[step], down_sem.at[step])

    tok_copy.start()
    for copy in small_copies:
        copy.start()
    for step in range(tp_count):
        for which, weight in enumerate((w_query, w_forget, w_input, w_outgate)):
            proj_copy(weight, step, which).start()
    state_copy.start()
    heads_copy.start()

    barrier = pltpu.get_barrier_semaphore()
    for step in range(1, group):
        pl.semaphore_signal(barrier, inc=1, device_id=coords(peer(step)), device_id_type=MESH)
    for step in range(group):
        gate_copy(step).start()
        up_copy(step).start()
    for step in range(group - 1, -1, -1):
        down_copy(step).start()
    per_cols = cols // LANES

    def proj_part(step, which):
        source = lax.rem(tp + tp_count - step, tp_count)
        first = (kv * tp_count + source) * per_cols
        gain_row = jnp.concatenate(
            [ngain_buf[pl.ds(first + i, 1), :] for i in range(per_cols)], axis=1
        )
        scaled = (tok_all[source].astype(jnp.float32) * gain_row).astype(jnp.bfloat16)
        proj_copy(w_query, step, which).wait()
        return jnp.dot(scaled, proj_w[step, which], preferred_element_type=jnp.float32)

    tok_copy.wait()
    for copy in small_copies:
        copy.wait()

    @pl.loop(0, 4)
    def _(which):
        proj_acc[which] = proj_part(0, which)

    pl.semaphore_wait(barrier, group - 1)
    tok_sends = []
    for step in range(1, tp_count):
        send = pltpu.make_async_remote_copy(
            src_ref=tok_all.at[tp],
            dst_ref=tok_all.at[tp],
            send_sem=tok_ssem.at[step],
            recv_sem=tok_rsem.at[step],
            device_id={"tp": lax.rem(tp + step, tp_count)},
            device_id_type=MESH,
        )
        send.start()
        tok_sends.append(send)
    for step in range(1, tp_count):
        source = lax.rem(tp + tp_count - step, tp_count)
        pltpu.make_async_remote_copy(
            src_ref=tok_all.at[source],
            dst_ref=tok_all.at[source],
            send_sem=tok_ssem.at[step],
            recv_sem=tok_rsem.at[step],
            device_id={"tp": source},
            device_id_type=MESH,
        ).wait_recv()

    squares = jnp.zeros((rows, 1), jnp.float32)
    for i in range(tp_count):
        block = tok_all[i].astype(jnp.float32)
        squares = squares + jnp.sum(block * block, axis=1, keepdims=True)
    square_send[...] = jnp.broadcast_to(squares, (rows, LANES))
    square_sends = []
    for step in range(kv_count - 1, 0, -1):
        send = pltpu.make_async_remote_copy(
            src_ref=square_send,
            dst_ref=square_recv.at[step],
            send_sem=square_ssem.at[step],
            recv_sem=square_rsem.at[step],
            device_id=coords(peer(step * tp_count)),
            device_id_type=MESH,
        )
        send.start()
        square_sends.append(send)

    @pl.loop(0, 4)
    def _(which):
        part = proj_acc[which]
        for step in range(1, tp_count):
            part = part + proj_part(step, which)
        for h in range(head_count):
            proj_float[:, which, h, :] = part[:, h * LANES : (h + 1) * LANES]

    proj_send[...] = proj_float[...].astype(jnp.bfloat16)
    proj_sends = []
    for step in range(kv_count - 1, 0, -1):
        target = peer(step * tp_count)
        send = pltpu.make_async_remote_copy(
            src_ref=proj_send.at[lax.div(target, tp_count)],
            dst_ref=proj_recv.at[step],
            send_sem=proj_ssem.at[step],
            recv_sem=proj_rsem.at[step],
            device_id=coords(target),
            device_id_type=MESH,
        )
        send.start()
        proj_sends.append(send)
    total = proj_float[kv]
    square_recv[0] = square_send[...]
    state_copy.wait()
    for step in range(1, kv_count):
        square_sends[kv_count - 1 - step].wait_recv()
    every_square = square_recv[0]
    for step in range(1, kv_count):
        every_square = every_square + square_recv[step]
    square_recv[0] = every_square
    row_scale = lax.rsqrt(square_recv[0, pl.ds(kv, 1), :] / width + epsilon)
    for step in range(1, kv_count):
        proj_sends[kv_count - 1 - step].wait_recv()
        total = total + proj_recv[step].astype(jnp.float32)
    query_act = silu(row_scale * total[0])
    lower = lower_buf[...]
    forget = lower + (1.0 - lower) / (1.0 + jnp.exp(-(row_scale * total[1])))
    key_in = 1.0 - forget
    value_in = row_scale * total[2]
    gate_act = silu(row_scale * total[3])
    forget_t = forget.T
    key_t = key_in.T
    query_t = query_act.T
    for h in range(head_count):
        fresh = forget_t[:, h : h + 1] * state_in[h] + key_t[:, h : h + 1] * value_in[h : h + 1, :]
        new_state[0, h] = fresh
        head_rows[h : h + 1, :] = jnp.sum(query_t[:, h : h + 1] * fresh, axis=0, keepdims=True)
    head_out = head_rows[...]
    head_out = head_out * lax.rsqrt(jnp.mean(head_out * head_out, axis=1, keepdims=True) + epsilon)
    gated_all[0] = (head_out * hgain_buf[...] * gate_act).astype(jnp.bfloat16)

    gated_sends = []
    for step in range(group - 1, 0, -1):
        send = pltpu.make_async_remote_copy(
            src_ref=gated_all.at[0],
            dst_ref=gated_all.at[step],
            send_sem=gated_ssem.at[step],
            recv_sem=gated_rsem.at[step],
            device_id=coords(peer(step)),
            device_id_type=MESH,
        )
        send.start()
        gated_sends.append(send)
    gated_float[kv, tp] = gated_all[0].astype(jnp.float32)
    heads_copy.wait()
    for step in range(1, group):
        gated_sends[group - 1 - step].wait_recv()
        source = peer(step)
        gated_float[lax.div(source, tp_count), lax.rem(source, tp_count)] = gated_all[step].astype(jnp.float32)
    every_head = jnp.concatenate(
        [gated_float[:, t, h, :] for t in range(tp_count) for h in range(head_count)], axis=1
    ).astype(jnp.bfloat16)
    mixed_add = jnp.dot(every_head, heads_w[...], preferred_element_type=jnp.float32)
    mixed = (tok_all[tp].astype(jnp.float32) + mixed_add).astype(jnp.bfloat16)
    mixed_all[0] = mixed

    mixed_sends = []
    for step in range(group - 1, 0, -1):
        send = pltpu.make_async_remote_copy(
            src_ref=mixed_all.at[0],
            dst_ref=mixed_all.at[step],
            send_sem=mixed_ssem.at[step],
            recv_sem=mixed_rsem.at[step],
            device_id=coords(peer(step)),
            device_id_type=MESH,
        )
        send.start()
        mixed_sends.append(send)

    gate_acc[...] = jnp.zeros_like(gate_acc)
    up_acc[...] = jnp.zeros_like(up_acc)

    def mixer_step(step, squares_sum):
        mixed_float = mixed_all[step].astype(jnp.float32)
        gain = jnp.concatenate(
            [mgain_buf[pl.ds(peer(step) * per_cols + i, 1), :] for i in range(per_cols)], axis=1
        )
        weighted = (mixed_float * gain).astype(jnp.bfloat16)
        gate_copy(step).wait()
        gate_acc[...] += jnp.dot(weighted, gate_w[step], preferred_element_type=jnp.float32)
        up_copy(step).wait()
        up_acc[...] += jnp.dot(weighted, up_w[step], preferred_element_type=jnp.float32)
        return squares_sum + jnp.sum(mixed_float * mixed_float, axis=1, keepdims=True)

    def mixer_arrived(step, squares_sum):
        pltpu.make_async_remote_copy(
            src_ref=mixed_all.at[0],
            dst_ref=mixed_all.at[step],
            send_sem=mixed_ssem.at[step],
            recv_sem=mixed_rsem.at[step],
            device_id=coords(peer(step)),
            device_id_type=MESH,
        ).wait_recv()
        return mixer_step(step, squares_sum)

    squares_sum = mixer_step(0, jnp.zeros((rows, 1), jnp.float32))
    squares_sum = lax.fori_loop(1, group, mixer_arrived, squares_sum)
    mixer_scale = lax.rsqrt(squares_sum / width + epsilon)
    hidden_buf[...] = (silu(mixer_scale * gate_acc[...]) * (mixer_scale * up_acc[...])).astype(jnp.bfloat16)

    def down_part(step):
        down_copy(step).wait()
        return jnp.dot(hidden_buf[...], down_w[step], preferred_element_type=jnp.float32)

    def red_send(step):
        return pltpu.make_async_remote_copy(
            src_ref=down_send.at[step],
            dst_ref=down_recv.at[step],
            send_sem=red_ssem.at[step],
            recv_sem=red_rsem.at[step],
            device_id=coords(peer(step)),
            device_id_type=MESH,
        )

    @pl.loop(1, group)
    def _(turn):
        step = group - turn
        down_send[step] = down_part(step).astype(jnp.bfloat16)
        red_send(step).start()

    final = mixed.astype(jnp.float32) + down_part(0)
    for step in range(1, group):
        red_send(step).wait_recv()
        final = final + down_recv[step].astype(jnp.float32)
    result[...] = final.astype(jnp.bfloat16)
    for send in tok_sends + square_sends + proj_sends + gated_sends + mixed_sends:
        send.wait_send()
    for step in range(1, group):
        red_send(step).wait_send()


def store_kernel(held, state, result, new_state, sems):
    copies = [
        pltpu.make_async_copy(held, result, sems.at[0]),
        pltpu.make_async_copy(state, new_state, sems.at[1]),
    ]
    for copy in copies:
        copy.start()
    for copy in copies:
        copy.wait()


def in_hbm(*arrays):
    return [pltpu.with_memory_space_constraint(array, pltpu.HBM) for array in arrays]


def local(
    kv_count,
    tp_count,
    tokens,
    rec_state,
    norm_gain,
    w_query,
    w_forget,
    w_input,
    w_outgate,
    lower_bound,
    head_gain,
    w_heads_out,
    mixer_gain,
    w_gate,
    w_up,
    w_down,
):
    group = kv_count * tp_count
    rows, cols = tokens.shape
    head_count = rec_state.shape[1]
    hidden = w_gate.shape[1]
    model_width = norm_gain.shape[0]
    head_width = head_count * HEAD_DIM
    fits = (
        rec_state.shape[0] == 1
        and group & (group - 1) == 0
        and tp_count & (tp_count - 1) == 0
        and HEAD_DIM == LANES
        and head_count % 8 == 0
        and cols % LANES == 0
        and hidden % LANES == 0
        and w_down.shape[0] == hidden
    )
    if not fits:
        return local_plain(
            tokens, rec_state, norm_gain, w_query, w_forget, w_input, w_outgate, lower_bound,
            head_gain, w_heads_out, mixer_gain, w_gate, w_up, w_down,
        )
    f32, bf16 = jnp.float32, jnp.bfloat16
    dma = pltpu.SemaphoreType.DMA
    vmem = pltpu.VMEM
    scratch = [
        vmem((tp_count, rows, cols), bf16),
        vmem(rec_state.shape[1:], f32),
        vmem((model_width // LANES, LANES), f32),
        vmem((head_count, LANES), f32),
        vmem((head_count, LANES), f32),
        vmem((model_width // LANES, LANES), f32),
        vmem((tp_count, 4, cols, w_query.shape[1]), bf16),
        vmem(w_heads_out.shape, bf16),
        vmem((group, cols, hidden), bf16),
        vmem((group, cols, hidden), bf16),
        vmem((group, hidden, cols), bf16),
        vmem((4, rows, w_query.shape[1]), f32),
        vmem((kv_count, 4, head_count, LANES), f32),
        vmem((kv_count, 4, head_count, LANES), bf16),
        vmem((kv_count, 4, head_count, LANES), bf16),
        vmem((rows, LANES), f32),
        vmem((kv_count, rows, LANES), f32),
        vmem((head_count, LANES), f32),
        vmem((group, head_count, LANES), bf16),
        vmem((kv_count, tp_count, head_count, LANES), f32),
        vmem((group, rows, cols), bf16),
        vmem((rows, hidden), f32),
        vmem((rows, hidden), f32),
        vmem((rows, hidden), bf16),
        vmem((group, rows, cols), bf16),
        vmem((group, rows, cols), bf16),
        dma((6,)),
        dma((tp_count, 4)),
        dma,
        dma((group,)),
        dma((group,)),
        dma((group,)),
        dma((tp_count,)),
        dma((tp_count,)),
        dma((kv_count,)),
        dma((kv_count,)),
        dma((kv_count,)),
        dma((kv_count,)),
        dma((group,)),
        dma((group,)),
        dma((group,)),
        dma((group,)),
        dma((group,)),
        dma((group,)),
    ]
    held, state = pl.pallas_call(
        functools.partial(layer_kernel, kv_count, tp_count),
        out_shape=(
            pltpu.VMEM(tokens.shape, bf16),
            pltpu.VMEM(rec_state.shape, f32),
        ),
        in_specs=[pl.BlockSpec(memory_space=pltpu.HBM)] * 14,
        out_specs=(
            pl.BlockSpec(memory_space=pltpu.VMEM),
            pl.BlockSpec(memory_space=pltpu.VMEM),
        ),
        scratch_shapes=scratch,
        compiler_params=pltpu.CompilerParams(
            collective_id=0, has_side_effects=True, vmem_limit_bytes=52 * 1024 * 1024
        ),
    )(
        *in_hbm(
        tokens,
        rec_state,
        norm_gain.reshape(-1, LANES),
        w_query,
        w_forget,
        w_input,
        w_outgate,
        lower_bound.reshape(-1, LANES),
        head_gain.reshape(-1, LANES),
        w_heads_out,
        mixer_gain.reshape(-1, LANES),
        w_gate,
        w_up,
        w_down,
        )
    )
    return pl.pallas_call(
        store_kernel,
        out_shape=(
            jax.ShapeDtypeStruct(tokens.shape, bf16),
            jax.ShapeDtypeStruct(rec_state.shape, f32),
        ),
        in_specs=[pl.BlockSpec(memory_space=pl.ANY)] * 2,
        out_specs=(pl.BlockSpec(memory_space=pl.ANY), pl.BlockSpec(memory_space=pl.ANY)),
        scratch_shapes=[dma((2,))],
    )(
        pltpu.with_memory_space_constraint(held, pltpu.VMEM),
        pltpu.with_memory_space_constraint(state, pltpu.VMEM),
    )


def solution(mesh):
    placed = (
        P("dp", ("kv", "tp")),
        P(("dp", "kv"), "tp", None, None),
        P(),
        P("kv", "tp"),
        P("kv", "tp"),
        P("kv", "tp"),
        P("kv", "tp"),
        P("tp"),
        P("tp"),
        P(None, ("kv", "tp")),
        P(),
        P(None, ("kv", "tp")),
        P(None, ("kv", "tp")),
        P(("kv", "tp"), None),
    )
    return jax.shard_map(
        functools.partial(local, mesh.shape["kv"], mesh.shape["tp"]),
        mesh=mesh,
        in_specs=placed,
        out_specs=(P("dp", ("kv", "tp")), P(("dp", "kv"), "tp", None, None)),
        check_vma=False,
    )
```
